32 devices in a mesh: fs: 8 (over z, y), tp: 4 (over x, core).
Axes of the slice: x: 2, y: 2, z: 4, core: 2. Of those that a mesh axis runs over, the one named last changes fastest.
Arguments:
- tokens: bfloat16 [4096, 2048], P(('fs', 'tp')), may hold values from -6 to 6
- norm_one: float32 [2048], replicated, may hold values from 0.1 to 1.9
- gate_one: bfloat16 [2048, 4608], P('fs', 'tp'), may hold values from -0.125 to 0.125
- up_one: bfloat16 [2048, 4608], P('fs', 'tp'), may hold values from -0.125 to 0.125
- down_one: bfloat16 [4608, 2048], P('tp', 'fs'), may hold values from -0.1875 to 0.1875
- norm_two: float32 [2048], replicated, may hold values from 0.1 to 1.9
- gate_two: bfloat16 [2048, 4608], P('fs', 'tp'), may hold values from -0.125 to 0.125
- up_two: bfloat16 [2048, 4608], P('fs', 'tp'), may hold values from -0.125 to 0.125
- down_two: bfloat16 [4608, 2048], P('tp', 'fs'), may hold values from -0.1875 to 0.1875
Outputs:
- result: bfloat16 [4096, 2048], P(('fs', 'tp'))
The draws below stay inside these ranges and needn't reach their ends.
All inputs are finite; a program needn't handle non-finite values.
Results may differ from the reference program's by a relative error of at most 0.015.
Values may be sent and summed in bfloat16 or wider, within the bound.
A program may use at most 64 MiB of HBM per device.

```python
import jax
import jax.numpy as jnp
from jax import lax

D = 2048
FF = 4608
TOKENS = 4096
N_FS = 8
N_TP = 4


def block_scale(stream_key, dims, pieces, least, largest):
    factor_of = 1.0
    for axis_at, parts in pieces:
        steps = jax.random.uniform(jax.random.fold_in(jax.random.fold_in(stream_key, 6), axis_at), (parts,), jnp.float32, least / len(pieces), largest / len(pieces))
        factor_of = factor_of * jnp.repeat(jnp.exp(steps), dims[axis_at] // parts).reshape((-1,) + (1,) * (len(dims) - 1 - axis_at))
    return factor_of


def bell_draw(own_key, dims, scale, bound, split=(), dtype=jnp.bfloat16):
    level = block_scale(own_key, dims, split, -0.22, 0.18) if split else 1.0
    drawn = jax.random.normal(own_key, dims, jnp.float32) * scale * level
    return jnp.minimum(jnp.maximum(drawn, -bound), bound).astype(dtype)


def setup_inputs(seed: int = 0) -> dict:
    key_list = jax.random.split(jax.random.key(seed), 10)
    return {
        "tokens": bell_draw(key_list[0], (TOKENS, D), 1.0, 6.0, ((0, 32),)),
        "norm_one": jnp.clip(1.0 + 0.18 * jax.random.normal(key_list[1], (D,), jnp.float32), 0.1, 1.9),
        "gate_one": bell_draw(key_list[2], (D, FF), D ** -0.5, 0.125, ((0, 8), (1, 4))),
        "up_one": bell_draw(key_list[3], (D, FF), D ** -0.5, 0.125, ((0, 8), (1, 4))),
        "down_one": bell_draw(key_list[4], (FF, D), (FF // 4) ** -0.5, 0.1875, ((0, 4), (1, 8))),
        "norm_two": jnp.clip(1.0 + 0.18 * jax.random.normal(key_list[5], (D,), jnp.float32), 0.1, 1.9),
        "gate_two": bell_draw(key_list[6], (D, FF), D ** -0.5, 0.125, ((0, 8), (1, 4))),
        "up_two": bell_draw(key_list[7], (D, FF), D ** -0.5, 0.125, ((0, 8), (1, 4))),
        "down_two": bell_draw(key_list[8], (FF, D), (FF // 4) ** -0.5, 0.1875, ((0, 4), (1, 8))),
    }


eps = 1e-06

def normalize(rows, gain):
    values = rows.astype(jnp.float32)
    scaled = values * lax.rsqrt(lax.optimization_barrier(jnp.mean(values * values, axis=-1, keepdims=True)) + eps)
    return (scaled * gain.astype(jnp.float32)).astype(jnp.bfloat16)

def product(left, right):
    return jnp.dot(left.astype(jnp.float32), right.astype(jnp.float32), preferred_element_type=jnp.float32)

def half_step(rows, gain, gate_w, up_w, down_w):
    normed = normalize(rows, gain)
    hidden = (jax.nn.silu(product(normed, gate_w)) * product(normed, up_w)).astype(jnp.bfloat16)
    width = down_w.shape[0] // N_TP
    total = jnp.zeros((rows.shape[0], down_w.shape[1]), jnp.float32)
    for block in range(N_TP):
        partial_value = product(hidden[:, block * width:(block + 1) * width], down_w[block * width:(block + 1) * width])
        rounded = lax.optimization_barrier(partial_value.astype(jnp.bfloat16))
        total = total + rounded.astype(jnp.float32)
    return (rows.astype(jnp.float32) + 0.5 * total).astype(jnp.bfloat16)

def reference(tokens, norm_one, gate_one, up_one, down_one, norm_two, gate_two, up_two, down_two):

    def group_step(rows):
        middle = half_step(rows, norm_one, gate_one, up_one, down_one)
        return half_step(middle, norm_two, gate_two, up_two, down_two)
    grouped = tokens.reshape(N_FS, tokens.shape[0] // N_FS, tokens.shape[1])
    return lax.map(group_step, grouped).reshape(tokens.shape)
```

```python
import functools

import jax
import jax.numpy as jnp
from jax import lax
from jax.experimental import pallas as pl
from jax.experimental.pallas import tpu as pltpu
from jax.sharding import PartitionSpec as P

eps = 1e-06
MESH = pl.DeviceIdType.MESH


def normalize(rows, gain):
    values = rows.astype(jnp.float32)
    scaled = values * lax.rsqrt(jnp.mean(values * values, axis=-1, keepdims=True) + eps)
    return (scaled * gain).astype(jnp.bfloat16)


def hidden_units(rows, gain, gate_w, up_w):
    normed = normalize(rows, gain)
    gate_full, up_full = (
        lax.all_gather(gate_w, "fs", axis=0, tiled=True),
        lax.all_gather(up_w, "fs", axis=0, tiled=True),
    )
    gate_sum = jnp.dot(normed, gate_full, preferred_element_type=jnp.float32)
    up_sum = jnp.dot(normed, up_full, preferred_element_type=jnp.float32)
    return (jax.nn.silu(gate_sum) * up_sum).astype(jnp.bfloat16)


def down_terms(hidden, down_w):
    return jnp.dot(
        hidden, lax.all_gather(down_w, "fs", axis=1, tiled=True), preferred_element_type=jnp.float32
    )


def plain_on_device(tokens, norm_one, gate_one, up_one, down_one, norm_two, gate_two, up_two, down_two):
    gathered = lax.all_gather(tokens, "tp", axis=0, tiled=True)
    first_terms = down_terms(hidden_units(gathered, norm_one, gate_one, up_one), down_one)
    summed = lax.psum(first_terms.astype(jnp.bfloat16), "tp").astype(jnp.float32)
    mid_group = (gathered.astype(jnp.float32) + 0.5 * summed).astype(jnp.bfloat16)
    mid_rows = lax.dynamic_slice_in_dim(
        mid_group, lax.axis_index("tp") * tokens.shape[0], tokens.shape[0], 0
    )
    second_terms = down_terms(hidden_units(mid_group, norm_two, gate_two, up_two), down_two)
    summed_two = lax.psum_scatter(
        second_terms.astype(jnp.bfloat16), "tp", scatter_dimension=0, tiled=True
    ).astype(jnp.float32)
    return (mid_rows.astype(jnp.float32) + 0.5 * summed_two).astype(jnp.bfloat16)


def kernel(
    nz, n_tp,
    tok_h, n1, g1_h, u1_h, d1_h, n2, g2_h, u2_h, d2_h,
    out,
    gu, dn, xs, mid, normed, gate, hidden, part, rs,
    loc_sem, tok_sem, w_recv, z_send, y_send, x_send, x_recv, m_send, m_recv, rs_send, rs_recv,
):
    fs, tp = lax.axis_index("fs"), lax.axis_index("tp")
    z, y = fs // 2, fs % 2
    oy = 1 - y
    n_fs = 2 * nz
    hbm = [g1_h, u1_h, d1_h, g2_h, u2_h, d2_h]
    n_w = len(hbm)
    rows, dim = tok_h.shape
    depth, width = g1_h.shape
    cols = d1_h.shape[1]
    gu_at = {0: 0, 1: 1, 3: 2, 4: 3}
    dn_at = {2: 0, 5: 1}

    gu_cut = depth - max(16, (depth * 3 // 16) // 16 * 16)
    dn_cut = width - max(16, (width // 6) // 16 * 16)

    def block(w, src):
        return gu.at[gu_at[w], src] if w in gu_at else dn.at[dn_at[w], src]

    def piece(w, src, p):
        cut, full = (gu_cut, depth) if w in gu_at else (dn_cut, width)
        return block(w, src).at[pl.ds(0, cut) if p == 0 else pl.ds(cut, full - cut)]

    def locals_(w):
        return pltpu.make_async_copy(hbm[w], block(w, fs), loc_sem.at[w])

    def z_copy(w, p, src, up):
        to = (z + 1 if up else z - 1) * 2 + y
        return pltpu.make_async_remote_copy(
            src_ref=piece(w, src, p), dst_ref=piece(w, src, p),
            send_sem=z_send.at[w, p, src, 1 if up else 0], recv_sem=w_recv.at[w, p, src],
            device_id=(to, tp), device_id_type=MESH)

    def y_copy(w, p, src):
        return pltpu.make_async_remote_copy(
            src_ref=piece(w, src, p), dst_ref=piece(w, src, p),
            send_sem=y_send.at[w, p, src // 2], recv_sem=w_recv.at[w, p, src],
            device_id=(z * 2 + oy, tp), device_id_type=MESH)

    def arrived(w, p, src):
        ref = piece(w, src, p)
        pltpu.make_async_copy(ref, ref, w_recv.at[w, p, src]).wait()

    def both_z(w, p, src):
        @pl.when(z < nz - 1)
        def _():
            z_copy(w, p, src, True).start()

        @pl.when(z > 0)
        def _():
            z_copy(w, p, src, False).start()

    def own_start(w):
        locals_(w).wait()
        y_copy(w, 1, fs).start()
        both_z(w, 0, fs)
        y_copy(w, 0, fs).start()
        both_z(w, 1, fs)

    def cross(w):
        src = z * 2 + oy
        arrived(w, 1, src)
        both_z(w, 1, src)

    def relay(w, d):
        def one(sz, going_up, more):
            own, other = sz * 2 + y, sz * 2 + oy
            for p, src in ((0, own), (1, own), (1, other)):
                arrived(w, p, src)

                @pl.when(more)
                def _():
                    z_copy(w, p, src, going_up).start()
                if p == 0:
                    y_copy(w, p, src).start()

        @pl.when(z - d >= 0)
        def _():
            one(z - d, True, z < nz - 1)

        @pl.when(z + d < nz)
        def _():
            one(z + d, False, z > 0)

    def at_distance(d, do):
        if d == 0:
            do(z)
        else:
            @pl.when(z - d >= 0)
            def _():
                do(z - d)

            @pl.when(z + d < nz)
            def _():
                do(z + d)

    def wait_other(w, d):
        at_distance(d, lambda sz: arrived(w, 0, sz * 2 + oy))

    def peer(j):
        return lax.rem(tp + j, n_tp)

    def x_copy(j):
        return pltpu.make_async_remote_copy(
            src_ref=xs.at[tp], dst_ref=xs.at[tp], send_sem=x_send.at[j], recv_sem=x_recv.at[tp],
            device_id=(fs, peer(j)), device_id_type=MESH)

    def m_copy(j):
        return pltpu.make_async_remote_copy(
            src_ref=mid.at[tp], dst_ref=mid.at[tp], send_sem=m_send.at[j], recv_sem=m_recv.at[tp],
            device_id=(fs, peer(j)), device_id_type=MESH)

    def rs_copy(h, j, src):
        return pltpu.make_async_remote_copy(
            src_ref=part.at[h, peer(j), src], dst_ref=rs.at[h, tp, src],
            send_sem=rs_send.at[h, j, src], recv_sem=rs_recv.at[h, tp, src],
            device_id=(fs, peer(j)), device_id_type=MESH)

    def norm_all(source, gain):
        @pl.loop(0, n_tp)
        def _(t):
            normed[pl.ds(pl.multiple_of(t * rows, rows), rows), :] = normalize(source[t], gain[...])

    step_cols = next(c for c in (384, 256, 128) if width % c == 0)

    def project(w, finish):
        at = gu_at[w]

        @pl.loop(0, width // step_cols)
        def _(i):
            c = pl.ds(pl.multiple_of(i * step_cols, step_cols), step_cols)
            weights = gu[at, :, :, c].reshape(dim, step_cols)
            finish(c, jnp.dot(normed[...], weights, preferred_element_type=jnp.float32))

    def keep_gate(c, value):
        gate[:, c] = value

    def keep_hidden(c, value):
        g = gate[:, c]
        hidden[:, c] = (g / (1.0 + jnp.exp(-g)) * value).astype(jnp.bfloat16)

    def down_block(h, src):
        value = jnp.dot(hidden[...], dn[h, src], preferred_element_type=jnp.float32).astype(jnp.bfloat16)
        for t in range(n_tp):
            part[h, t, src] = value[t * rows:(t + 1) * rows]

    def rs_start(h, src):
        for j in range(1, n_tp):
            rs_copy(h, j, src).start()

    def finish(h, base, store):
        @pl.loop(0, n_fs)
        def _(src):
            total = part[h, tp, src].astype(jnp.float32)
            for j in range(1, n_tp):
                ref = rs.at[h, peer(j), src]
                pltpu.make_async_copy(ref, ref, rs_recv.at[h, peer(j), src]).wait()
                total = total + rs[h, peer(j), src].astype(jnp.float32)
            c = pl.ds(pl.multiple_of(src * cols, cols), cols)
            store(c, (base[tp, :, c].astype(jnp.float32) + 0.5 * total).astype(jnp.bfloat16))

    tok_local = pltpu.make_async_copy(tok_h, xs.at[tp], tok_sem)
    locals_(0).start()
    tok_local.start()
    for w in range(1, n_w):
        locals_(w).start()
    barrier = pltpu.get_barrier_semaphore()
    pl.semaphore_signal(barrier, inc=1, device_id=(z * 2 + oy, tp), device_id_type=MESH)
    for j in range(1, n_tp):
        pl.semaphore_signal(barrier, inc=1, device_id=(fs, peer(j)), device_id_type=MESH)

    @pl.when(z < nz - 1)
    def _():
        pl.semaphore_signal(barrier, inc=1, device_id=((z + 1) * 2 + y, tp), device_id_type=MESH)

    @pl.when(z > 0)
    def _():
        pl.semaphore_signal(barrier, inc=1, device_id=((z - 1) * 2 + y, tp), device_id_type=MESH)

    neighbours = (z + nz - 1) // nz + (2 * nz - 2 - z) // nz
    pl.semaphore_wait(barrier, n_tp + neighbours)

    own_start(0)
    tok_local.wait()
    for j in range(1, n_tp):
        x_copy(j).start()

    def wait_mid():
        for j in range(1, n_tp):
            ref = mid.at[peer(j)]
            pltpu.make_async_copy(ref, ref, m_recv.at[peer(j)]).wait()

    def compute(w):
        if w == 0:
            for j in range(1, n_tp):
                ref = xs.at[peer(j)]
                pltpu.make_async_copy(ref, ref, x_recv.at[peer(j)]).wait()
            norm_all(xs, n1)
            project(w, keep_gate)
        elif w == 3:
            wait_mid()
            norm_all(mid, n2)
            project(w, keep_gate)
        elif w in (1, 4):
            project(w, keep_hidden)
        elif w == 2:
            @pl.loop(0, n_fs)
            def _(src):
                down_block(0, src)
                rs_start(0, src)

    def down_own(d):
        def do(sz):
            down_block(1, sz * 2 + y)
            rs_start(1, sz * 2 + y)
        at_distance(d, do)

    def down_other(d):
        def do(sz):
            arrived(5, 0, sz * 2 + oy)
            down_block(1, sz * 2 + oy)
            rs_start(1, sz * 2 + oy)
        at_distance(d, do)

    def full(w):
        for d in range(nz):
            wait_other(w, d)
        compute(w)

    last = n_w - 1

    def store_mid(c, value):
        mid[tp, :, c] = value

    def store_out(c, value):
        out[:, c] = value

    for s in range(n_w + nz - 2):
        if s + 1 < n_w:
            own_start(s + 1)
        if s == 3 + nz:
            finish(0, xs, store_mid)
            for j in range(1, n_tp):
                m_copy(j).start()
        for d in range(nz - 1, 0, -1):
            if 0 <= s - d < n_w:
                relay(s - d, d)
        if s < n_w:
            cross(s)
        if 0 <= s - nz < n_w:
            full(s - nz)
    full(last - 1)
    for d in range(nz - 1):
        down_own(d)
        if d < nz - 2:
            down_other(d)
    relay(last, nz - 1)
    down_own(nz - 1)
    down_other(nz - 2)
    down_other(nz - 1)
    finish(1, mid, store_out)

    def sent_z(w, p, src, up):
        pltpu.make_async_copy(piece(w, src, p), piece(w, src, p), z_send.at[w, p, src, 1 if up else 0]).wait()

    for w in range(n_w):
        for p in range(2):
            for sz in range(nz):
                if p == 0:
                    ref = piece(w, sz * 2 + y, 0)
                    pltpu.make_async_copy(ref, ref, y_send.at[w, 0, sz]).wait()
                for sy in ((y,) if p == 0 else (y, oy)):
                    src = sz * 2 + sy

                    @pl.when((z >= sz) & (z < nz - 1))
                    def _():
                        sent_z(w, p, src, True)

                    @pl.when((z <= sz) & (z > 0))
                    def _():
                        sent_z(w, p, src, False)
        ref = piece(w, fs, 1)
        pltpu.make_async_copy(ref, ref, y_send.at[w, 1, z]).wait()
    for j in range(1, n_tp):
        x_copy(j).wait_send()
        m_copy(j).wait_send()

        @pl.loop(0, n_fs)
        def _(src):
            for h in range(2):
                rs_copy(h, j, src).wait_send()


def line_on_device(nz, n_tp, tokens, norm_one, gate_one, up_one, down_one, norm_two, gate_two, up_two, down_two):
    rows, dim = tokens.shape
    depth, width = gate_one.shape
    cols = down_one.shape[1]
    n_fs, group = 2 * nz, n_tp * rows
    bf, f32 = jnp.bfloat16, jnp.float32
    hbm, vmem = pl.BlockSpec(memory_space=pl.ANY), pl.BlockSpec(memory_space=pltpu.VMEM)
    dma = pltpu.SemaphoreType.DMA
    return pl.pallas_call(
        functools.partial(kernel, nz, n_tp),
        out_shape=jax.ShapeDtypeStruct((rows, dim), bf),
        in_specs=[hbm, vmem, hbm, hbm, hbm, vmem, hbm, hbm, hbm],
        out_specs=vmem,
        scratch_shapes=[
            pltpu.VMEM((4, n_fs, depth, width), bf),
            pltpu.VMEM((2, n_fs, width, cols), bf),
            pltpu.VMEM((n_tp, rows, dim), bf),
            pltpu.VMEM((n_tp, rows, dim), bf),
            pltpu.VMEM((group, dim), bf),
            pltpu.VMEM((group, width), f32),
            pltpu.VMEM((group, width), bf),
            pltpu.VMEM((2, n_tp, n_fs, rows, cols), bf),
            pltpu.VMEM((2, n_tp, n_fs, rows, cols), bf),
            dma((6,)), dma,
            dma((6, 2, n_fs)), dma((6, 2, n_fs, 2)), dma((6, 2, nz)),
            dma((n_tp,)), dma((n_tp,)), dma((n_tp,)), dma((n_tp,)),
            dma((2, n_tp, n_fs)), dma((2, n_tp, n_fs)),
        ],
        compiler_params=pltpu.CompilerParams(
            collective_id=0, has_side_effects=True, vmem_limit_bytes=66_000_000
        ),
    )(tokens, norm_one.reshape(1, -1), gate_one, up_one, down_one,
      norm_two.reshape(1, -1), gate_two, up_two, down_two)


def pairs_along_y(mesh):
    line = [d.coords for d in mesh.devices[:, 0]]
    if len(line) % 2 or len(line) < 6:
        return False
    nz = len(line) // 2
    return all(
        line[2 * k][2] == line[2 * k + 1][2] == line[0][2] + k
        and line[2 * k + 1][1] == line[2 * k][1] + 1 == line[0][1] + 1
        for k in range(nz)
    )


def solution(mesh):
    n_fs, n_tp = mesh.shape["fs"], mesh.shape["tp"]
    body = functools.partial(line_on_device, n_fs // 2, n_tp) if pairs_along_y(mesh) else plain_on_device
    return jax.shard_map(
        body,
        mesh=mesh,
        in_specs=(
            P(("fs", "tp"), None),
            P(),
            P("fs", "tp"),
            P("fs", "tp"),
            P("tp", "fs"),
            P(),
            P("fs", "tp"),
            P("fs", "tp"),
            P("tp", "fs"),
        ),
        out_specs=P(("fs", "tp"), None),
        check_vma=False,
    )
```

```python
import functools

import jax
import jax.numpy as jnp
from jax import lax
from jax.experimental import pallas as pl
from jax.experimental.pallas import tpu as pltpu
from jax.sharding import PartitionSpec as P

eps = 1e-06
MESH = pl.DeviceIdType.MESH


def normalize(rows, gain):
    values = rows.astype(jnp.float32)
    scaled = values * lax.rsqrt(jnp.mean(values * values, axis=-1, keepdims=True) + eps)
    return (scaled * gain).astype(jnp.bfloat16)


def hidden_units(rows, gain, gate_w, up_w):
    normed = normalize(rows, gain)
    gate_full, up_full = (
        lax.all_gather(gate_w, "fs", axis=0, tiled=True),
        lax.all_gather(up_w, "fs", axis=0, tiled=True),
    )
    gate_sum = jnp.dot(normed, gate_full, preferred_element_type=jnp.float32)
    up_sum = jnp.dot(normed, up_full, preferred_element_type=jnp.float32)
    return (jax.nn.silu(gate_sum) * up_sum).astype(jnp.bfloat16)


def down_terms(hidden, down_w):
    return jnp.dot(
        hidden, lax.all_gather(down_w, "fs", axis=1, tiled=True), preferred_element_type=jnp.float32
    )


def plain_on_device(tokens, norm_one, gate_one, up_one, down_one, norm_two, gate_two, up_two, down_two):
    gathered = lax.all_gather(tokens, "tp", axis=0, tiled=True)
    first_terms = down_terms(hidden_units(gathered, norm_one, gate_one, up_one), down_one)
    summed = lax.psum(first_terms.astype(jnp.bfloat16), "tp").astype(jnp.float32)
    mid_group = (gathered.astype(jnp.float32) + 0.5 * summed).astype(jnp.bfloat16)
    mid_rows = lax.dynamic_slice_in_dim(
        mid_group, lax.axis_index("tp") * tokens.shape[0], tokens.shape[0], 0
    )
    second_terms = down_terms(hidden_units(mid_group, norm_two, gate_two, up_two), down_two)
    summed_two = lax.psum_scatter(
        second_terms.astype(jnp.bfloat16), "tp", scatter_dimension=0, tiled=True
    ).astype(jnp.float32)
    return (mid_rows.astype(jnp.float32) + 0.5 * summed_two).astype(jnp.bfloat16)


def kernel(
    nz, n_tp,
    tok_h, n1, g1_h, u1_h, d1_h, n2, g2_h, u2_h, d2_h,
    out,
    gu, dn, xs, mid, normed, gate, hidden, part, rs,
    loc_sem, tok_sem, w_recv, z_send, y_send, x_send, x_recv, m_send, m_recv, rs_send, rs_recv,
):
    fs, tp = lax.axis_index("fs"), lax.axis_index("tp")
    z, y = fs // 2, fs % 2
    oy = 1 - y
    n_fs = 2 * nz
    hbm = [g1_h, u1_h, d1_h, g2_h, u2_h, d2_h]
    n_w = len(hbm)
    rows, dim = tok_h.shape
    depth, width = g1_h.shape
    cols = d1_h.shape[1]
    gu_at = {0: 0, 1: 1, 3: 2, 4: 3}
    dn_at = {2: 0, 5: 1}

    shares = (2, 2, 2, 2, 3, 3)

    def cut_of(w, full):
        return full - max(16, full * shares[w] // 256 * 16)

    def block(w, src):
        return gu.at[gu_at[w], src] if w in gu_at else dn.at[dn_at[w], src]

    def piece(w, src, p):
        full = depth if w in gu_at else width
        cut = cut_of(w, full)
        return block(w, src).at[pl.ds(0, cut) if p == 0 else pl.ds(cut, full - cut)]

    def locals_(w):
        return pltpu.make_async_copy(hbm[w], block(w, fs), loc_sem.at[w])

    def z_copy(w, p, src, up):
        to = (z + 1 if up else z - 1) * 2 + y
        return pltpu.make_async_remote_copy(
            src_ref=piece(w, src, p), dst_ref=piece(w, src, p),
            send_sem=z_send.at[w, p, src, 1 if up else 0], recv_sem=w_recv.at[w, p, src],
            device_id=(to, tp), device_id_type=MESH)

    def y_copy(w, p, src):
        return pltpu.make_async_remote_copy(
            src_ref=piece(w, src, p), dst_ref=piece(w, src, p),
            send_sem=y_send.at[w, p, src // 2], recv_sem=w_recv.at[w, p, src],
            device_id=(z * 2 + oy, tp), device_id_type=MESH)

    def arrived(w, p, src):
        ref = piece(w, src, p)
        pltpu.make_async_copy(ref, ref, w_recv.at[w, p, src]).wait()

    def both_z(w, p, src):
        @pl.when(z < nz - 1)
        def _():
            z_copy(w, p, src, True).start()

        @pl.when(z > 0)
        def _():
            z_copy(w, p, src, False).start()

    def own_start(w):
        locals_(w).wait()
        y_copy(w, 1, fs).start()
        both_z(w, 0, fs)
        y_copy(w, 0, fs).start()
        both_z(w, 1, fs)

    def cross(w):
        src = z * 2 + oy
        arrived(w, 1, src)
        both_z(w, 1, src)

    def relay(w, d):
        def one(sz, going_up, more):
            own, other = sz * 2 + y, sz * 2 + oy
            for p, src in ((0, own), (1, own), (1, other)):
                arrived(w, p, src)

                @pl.when(more)
                def _():
                    z_copy(w, p, src, going_up).start()
                if p == 0:
                    y_copy(w, p, src).start()

        @pl.when(z - d >= 0)
        def _():
            one(z - d, True, z < nz - 1)

        @pl.when(z + d < nz)
        def _():
            one(z + d, False, z > 0)

    def at_distance(d, do):
        if d == 0:
            do(z)
        else:
            @pl.when(z - d >= 0)
            def _():
                do(z - d)

            @pl.when(z + d < nz)
            def _():
                do(z + d)

    def wait_other(w, d):
        at_distance(d, lambda sz: arrived(w, 0, sz * 2 + oy))

    def peer(j):
        return lax.rem(tp + j, n_tp)

    def x_copy(j):
        return pltpu.make_async_remote_copy(
            src_ref=xs.at[tp], dst_ref=xs.at[tp], send_sem=x_send.at[j], recv_sem=x_recv.at[tp],
            device_id=(fs, peer(j)), device_id_type=MESH)

    def m_copy(j):
        return pltpu.make_async_remote_copy(
            src_ref=mid.at[tp], dst_ref=mid.at[tp], send_sem=m_send.at[j], recv_sem=m_recv.at[tp],
            device_id=(fs, peer(j)), device_id_type=MESH)

    def rs_copy(h, j, src):
        return pltpu.make_async_remote_copy(
            src_ref=part.at[h, peer(j), src], dst_ref=rs.at[h, tp, src],
            send_sem=rs_send.at[h, j, src], recv_sem=rs_recv.at[h, tp, src],
            device_id=(fs, peer(j)), device_id_type=MESH)

    def norm_all(source, gain):
        @pl.loop(0, n_tp)
        def _(t):
            normed[pl.ds(pl.multiple_of(t * rows, rows), rows), :] = normalize(source[t], gain[...])

    step_cols = next(c for c in (384, 256, 128) if width % c == 0)

    def project(w, finish):
        at = gu_at[w]

        @pl.loop(0, width // step_cols)
        def _(i):
            c = pl.ds(pl.multiple_of(i * step_cols, step_cols), step_cols)
            weights = gu[at, :, :, c].reshape(dim, step_cols)
            finish(c, jnp.dot(normed[...], weights, preferred_element_type=jnp.float32))

    def keep_gate(c, value):
        gate[:, c] = value

    def keep_hidden(c, value):
        g = gate[:, c]
        hidden[:, c] = (g / (1.0 + jnp.exp(-g)) * value).astype(jnp.bfloat16)

    def down_block(h, src):
        value = jnp.dot(hidden[...], dn[h, src], preferred_element_type=jnp.float32).astype(jnp.bfloat16)
        for t in range(n_tp):
            part[h, t, src] = value[t * rows:(t + 1) * rows]

    def rs_start(h, src):
        for j in range(1, n_tp):
            rs_copy(h, j, src).start()

    def finish(h, base, store):
        @pl.loop(0, n_fs)
        def _(src):
            total = part[h, tp, src].astype(jnp.float32)
            for j in range(1, n_tp):
                ref = rs.at[h, peer(j), src]
                pltpu.make_async_copy(ref, ref, rs_recv.at[h, peer(j), src]).wait()
                total = total + rs[h, peer(j), src].astype(jnp.float32)
            c = pl.ds(pl.multiple_of(src * cols, cols), cols)
            store(c, (base[tp, :, c].astype(jnp.float32) + 0.5 * total).astype(jnp.bfloat16))

    tok_local = pltpu.make_async_copy(tok_h, xs.at[tp], tok_sem)
    locals_(0).start()
    tok_local.start()
    for w in range(1, n_w):
        locals_(w).start()
    barrier = pltpu.get_barrier_semaphore()
    pl.semaphore_signal(barrier, inc=1, device_id=(z * 2 + oy, tp), device_id_type=MESH)
    for j in range(1, n_tp):
        pl.semaphore_signal(barrier, inc=1, device_id=(fs, peer(j)), device_id_type=MESH)

    @pl.when(z < nz - 1)
    def _():
        pl.semaphore_signal(barrier, inc=1, device_id=((z + 1) * 2 + y, tp), device_id_type=MESH)

    @pl.when(z > 0)
    def _():
        pl.semaphore_signal(barrier, inc=1, device_id=((z - 1) * 2 + y, tp), device_id_type=MESH)

    neighbours = (z + nz - 1) // nz + (2 * nz - 2 - z) // nz
    pl.semaphore_wait(barrier, n_tp + neighbours)

    own_start(0)
    tok_local.wait()
    for j in range(1, n_tp):
        x_copy(j).start()

    def wait_mid():
        for j in range(1, n_tp):
            ref = mid.at[peer(j)]
            pltpu.make_async_copy(ref, ref, m_recv.at[peer(j)]).wait()

    def compute(w):
        if w == 0:
            for j in range(1, n_tp):
                ref = xs.at[peer(j)]
                pltpu.make_async_copy(ref, ref, x_recv.at[peer(j)]).wait()
            norm_all(xs, n1)
            project(w, keep_gate)
        elif w == 3:
            wait_mid()
            norm_all(mid, n2)
            project(w, keep_gate)
        elif w in (1, 4):
            project(w, keep_hidden)
        elif w == 2:
            @pl.loop(0, n_fs)
            def _(src):
                down_block(0, src)
                rs_start(0, src)

    def down_own(d):
        def do(sz):
            down_block(1, sz * 2 + y)
            rs_start(1, sz * 2 + y)
        at_distance(d, do)

    def down_other(d):
        def do(sz):
            arrived(5, 0, sz * 2 + oy)
            down_block(1, sz * 2 + oy)
            rs_start(1, sz * 2 + oy)
        at_distance(d, do)

    def full(w):
        for d in range(nz):
            wait_other(w, d)
        compute(w)

    last = n_w - 1

    def store_mid(c, value):
        mid[tp, :, c] = value

    def store_out(c, value):
        out[:, c] = value

    for w in range(1, 2):
        own_start(w)
    for s in range(n_w + nz - 2):
        if s + 2 < n_w:
            own_start(s + 2)
        for d in range(nz - 1, 0, -1):
            if 0 <= s - d < n_w:
                relay(s - d, d)
        if s < n_w:
            cross(s)
        if s == 2 + nz:
            finish(0, xs, store_mid)
            for j in range(1, n_tp):
                m_copy(j).start()
        elif s == 3 + nz:
            full(3)
            full(4)
        elif 0 <= s - nz + 1 < n_w:
            full(s - nz + 1)
    for d in range(nz - 1):
        down_own(d)
        if d < nz - 2:
            down_other(d)
    relay(last, nz - 1)
    down_own(nz - 1)
    down_other(nz - 2)
    down_other(nz - 1)
    finish(1, mid, store_out)

    def sent_z(w, p, src, up):
        pltpu.make_async_copy(piece(w, src, p), piece(w, src, p), z_send.at[w, p, src, 1 if up else 0]).wait()

    for w in range(n_w):
        for p in range(2):
            for sz in range(nz):
                if p == 0:
                    ref = piece(w, sz * 2 + y, 0)
                    pltpu.make_async_copy(ref, ref, y_send.at[w, 0, sz]).wait()
                for sy in ((y,) if p == 0 else (y, oy)):
                    src = sz * 2 + sy

                    @pl.when((z >= sz) & (z < nz - 1))
                    def _():
                        sent_z(w, p, src, True)

                    @pl.when((z <= sz) & (z > 0))
                    def _():
                        sent_z(w, p, src, False)
        ref = piece(w, fs, 1)
        pltpu.make_async_copy(ref, ref, y_send.at[w, 1, z]).wait()
    for j in range(1, n_tp):
        x_copy(j).wait_send()
        m_copy(j).wait_send()

        @pl.loop(0, n_fs)
        def _(src):
            for h in range(2):
                rs_copy(h, j, src).wait_send()


def line_on_device(nz, n_tp, tokens, norm_one, gate_one, up_one, down_one, norm_two, gate_two, up_two, down_two):
    rows, dim = tokens.shape
    depth, width = gate_one.shape
    cols = down_one.shape[1]
    n_fs, group = 2 * nz, n_tp * rows
    bf, f32 = jnp.bfloat16, jnp.float32
    hbm, vmem = pl.BlockSpec(memory_space=pl.ANY), pl.BlockSpec(memory_space=pltpu.VMEM)
    dma = pltpu.SemaphoreType.DMA
    return pl.pallas_call(
        functools.partial(kernel, nz, n_tp),
        out_shape=jax.ShapeDtypeStruct((rows, dim), bf),
        in_specs=[hbm, vmem, hbm, hbm, hbm, vmem, hbm, hbm, hbm],
        out_specs=vmem,
        scratch_shapes=[
            pltpu.VMEM((4, n_fs, depth, width), bf),
            pltpu.VMEM((2, n_fs, width, cols), bf),
            pltpu.VMEM((n_tp, rows, dim), bf),
            pltpu.VMEM((n_tp, rows, dim), bf),
            pltpu.VMEM((group, dim), bf),
            pltpu.VMEM((group, width), f32),
            pltpu.VMEM((group, width), bf),
            pltpu.VMEM((2, n_tp, n_fs, rows, cols), bf),
            pltpu.VMEM((2, n_tp, n_fs, rows, cols), bf),
            dma((6,)), dma,
            dma((6, 2, n_fs)), dma((6, 2, n_fs, 2)), dma((6, 2, nz)),
            dma((n_tp,)), dma((n_tp,)), dma((n_tp,)), dma((n_tp,)),
            dma((2, n_tp, n_fs)), dma((2, n_tp, n_fs)),
        ],
        compiler_params=pltpu.CompilerParams(
            collective_id=0, has_side_effects=True, vmem_limit_bytes=66_000_000
        ),
    )(tokens, norm_one.reshape(1, -1), gate_one, up_one, down_one,
      norm_two.reshape(1, -1), gate_two, up_two, down_two)


def pairs_along_y(mesh):
    line = [d.coords for d in mesh.devices[:, 0]]
    if len(line) % 2 or len(line) < 6:
        return False
    nz = len(line) // 2
    return all(
        line[2 * k][2] == line[2 * k + 1][2] == line[0][2] + k
        and line[2 * k + 1][1] == line[2 * k][1] + 1 == line[0][1] + 1
        for k in range(nz)
    )


def solution(mesh):
    n_fs, n_tp = mesh.shape["fs"], mesh.shape["tp"]
    body = functools.partial(line_on_device, n_fs // 2, n_tp) if pairs_along_y(mesh) else plain_on_device
    return jax.shard_map(
        body,
        mesh=mesh,
        in_specs=(
            P(("fs", "tp"), None),
            P(),
            P("fs", "tp"),
            P("fs", "tp"),
            P("tp", "fs"),
            P(),
            P("fs", "tp"),
            P("fs", "tp"),
            P("tp", "fs"),
        ),
        out_specs=P(("fs", "tp"), None),
        check_vma=False,
    )
```
